32 devices in a mesh: fs: 8 (over z, x), tp: 4 (over y, core).
Axes of the slice: x: 2, y: 2, z: 4, core: 2. Of those that a mesh axis runs over, the one named last changes fastest.
Arguments:
- normed_inputs: bfloat16 [24576, 2048], P(('fs', 'tp')), may hold values from -6 to 6
- query_cotangent: bfloat16 [24576, 1024], P(('fs', 'tp')), may hold values from -6 to 6
- head_outputs: bfloat16 [24576, 1024], P(('fs', 'tp')), may hold values from -6 to 6
- output_cotangent: bfloat16 [24576, 2048], P(('fs', 'tp')), may hold values from -6 to 6
- query_weight: float32 [2048, 1024], P('fs', 'tp'), may hold values from -0.125 to 0.125
- out_weight: float32 [1024, 2048], P('fs', 'tp'), may hold values from -0.1875 to 0.1875
- query_basis: bfloat16 [2048, 512], P('fs'), may hold values from -0.125 to 0.125
- out_basis: bfloat16 [1024, 512], P('fs'), may hold values from -0.1875 to 0.1875
- query_mean: float32 [512, 1024], P('fs', 'tp'), may hold values from -6 to 6
- query_square: float32 [512, 1024], P('fs', 'tp'), may hold values from 0.5 to 2
- out_mean: float32 [512, 2048], P('fs', 'tp'), may hold values from -6 to 6
- out_square: float32 [512, 2048], P('fs', 'tp'), may hold values from 0.5 to 2
Outputs:
- query_mean_new: float32 [512, 1024], P('fs', 'tp')
- query_square_new: float32 [512, 1024], P('fs', 'tp')
- query_step: float32 [2048, 1024], P('fs', 'tp')
- query_weight_new: float32 [2048, 1024], P('fs', 'tp')
- query_copy: bfloat16 [2048, 1024], P(None, 'tp')
- out_mean_new: float32 [512, 2048], P('fs', 'tp')
- out_square_new: float32 [512, 2048], P('fs', 'tp')
- out_step: float32 [1024, 2048], P('fs', 'tp')
- out_weight_new: float32 [1024, 2048], P('fs', 'tp')
- out_copy: bfloat16 [1024, 2048], P(None, 'tp')
The draws below stay inside these ranges and needn't reach their ends.
All inputs are finite; a program needn't handle non-finite values.
Results may differ from the reference program's by a relative error of at most 0.009.
Values may be sent and summed in bfloat16 or wider, within the bound.
No kernel may reach another device: no remote copies, remote signals or barrier semaphores. Data moves between devices by JAX's collectives and lax.ppermute only.
A program may use at most 64 MiB of HBM per device.

```python
import math
import jax
import jax.numpy as jnp
from jax import lax

D = 2048
QW = 1024
RANK = 512
TOK_DEV = 768
TOKENS = 24576


def strengthened(array, stream_key, source, target, blocks, factor):
    def block_of(position):
        return (jnp.arange(array.shape[position]) // (array.shape[position] // blocks)).reshape((-1,) + (1,) * (array.ndim - 1 - position))

    one_side = jax.random.permutation(stream_key, blocks)[block_of(target)]
    second = (block_of(target) + blocks // 2) % blocks
    return jnp.where((block_of(source) == one_side) | (block_of(source) == second), factor * array, array)


def block_scale(own_key, extent, shards, least, top_value):
    loudness, own = 1.0, jax.random.fold_in(own_key, 6)
    for axis_at, shards_of in shards:
        heights = jnp.exp(jax.random.uniform(jax.random.fold_in(own, axis_at), (shards_of,), jnp.float32, least / len(shards), top_value / len(shards)))
        loudness = loudness * jnp.repeat(heights, extent[axis_at] // shards_of).reshape([-1 if axis == axis_at else 1 for axis in range(len(extent))])
    return loudness


def normal_values(own_key, extent, deviation, reach, cuts=(), kind=jnp.bfloat16):
    loudness = block_scale(own_key, extent, cuts, -0.22, 0.18) if cuts else 1.0
    result = jax.random.normal(own_key, extent, jnp.float32) * deviation * loudness
    return jnp.minimum(jnp.maximum(result, -reach), reach).astype(kind)


def heavy_noise(stream_key, dims, scale, limit, shards, heavy, dtype=jnp.bfloat16):
    result = scale * jax.random.normal(stream_key, dims, jnp.float32)
    if shards:
        result = result * block_scale(stream_key, dims, shards, -0.22, 0.18)
    return jnp.clip(strengthened(result, jax.random.fold_in(stream_key, 3), *heavy), -limit, limit).astype(dtype)


def setup_inputs(seed: int = 0) -> dict:
    seeds = jax.random.split(jax.random.key(seed), 13)
    normed_inputs = heavy_noise(seeds[0], (TOKENS, D), 1.0, 6.0, ((0, 32),), (0, 1, 32, 2.75))
    query_cotangent = normal_values(seeds[1], (TOKENS, QW), 1.0, 6.0, ((0, 32),))
    head_outputs = heavy_noise(seeds[2], (TOKENS, QW), 1.0, 6.0, ((0, 32),), (0, 1, 32, 2.75))
    output_cotangent = normal_values(seeds[3], (TOKENS, D), 1.0, 6.0, ((0, 32),))
    query_weight = normal_values(seeds[4], (D, QW), D ** -0.5, 0.125, ((0, 8), (1, 4)), jnp.float32)
    out_weight = normal_values(seeds[5], (QW, D), QW ** -0.5, 0.1875, ((0, 8), (1, 4)), jnp.float32)
    query_basis = normal_values(seeds[6], (D, RANK), D ** -0.5, 0.125, ((0, 8),))
    out_basis = normal_values(seeds[7], (QW, RANK), QW ** -0.5, 0.1875, ((0, 8),))
    query_mean = normal_values(seeds[8], (RANK, QW), 1.0, 6.0, ((0, 8), (1, 4)), jnp.float32)
    query_square = jnp.clip(jnp.exp(math.log(2.0) - 1.3862944 * jax.random.uniform(seeds[9], (RANK, QW), jnp.float32) ** block_scale(seeds[9], (RANK, QW), ((0, 8), (1, 4)), -0.2, 0.2)), 0.5, 2.0)
    out_mean = normal_values(seeds[10], (RANK, D), 1.0, 6.0, ((0, 8), (1, 4)), jnp.float32)
    out_square = jnp.clip(jnp.exp(math.log(2.0) - 1.3862944 * jax.random.uniform(seeds[11], (RANK, D), jnp.float32) ** block_scale(seeds[11], (RANK, D), ((0, 8), (1, 4)), -0.2, 0.2)), 0.5, 2.0)
    return dict(normed_inputs=normed_inputs, query_cotangent=query_cotangent, head_outputs=head_outputs, output_cotangent=output_cotangent, query_weight=query_weight, out_weight=out_weight, query_basis=query_basis, out_basis=out_basis, query_mean=query_mean, query_square=query_square, out_mean=out_mean, out_square=out_square)


def update_matrix(grad, basis, mean, square, weight):
    wide_basis = basis.astype(jnp.float32)
    reduced = jnp.dot(wide_basis.T, grad, precision=lax.Precision.HIGHEST)
    mean_new = 0.8 * mean + 0.2 * reduced
    square_new = 0.9 * square + 0.1 * reduced * reduced
    direction = mean_new / (jnp.sqrt(square_new) + 1e-08)
    full = jnp.dot(wide_basis, direction, precision=lax.Precision.HIGHEST)
    step = full * lax.rsqrt(lax.optimization_barrier(jnp.mean(full * full, axis=0)) + 0.05)
    weight_new = weight - 0.01 * step
    return (mean_new, square_new, step, weight_new, weight_new.astype(jnp.bfloat16))

def reference(normed_inputs, query_cotangent, head_outputs, output_cotangent, query_weight, out_weight, query_basis, out_basis, query_mean, query_square, out_mean, out_square):
    blocks = TOKENS // TOK_DEV
    inputs_blocks = normed_inputs.reshape(blocks, TOK_DEV, D)
    query_blocks = query_cotangent.reshape(blocks, TOK_DEV, QW)
    heads_blocks = head_outputs.reshape(blocks, TOK_DEV, QW)
    output_blocks = output_cotangent.reshape(blocks, TOK_DEV, D)

    def accumulate(totals, pieces):
        inputs_part, query_part, heads_part, output_part = pieces
        query_total = totals[0] + jnp.dot(inputs_part.astype(jnp.float32).T, query_part.astype(jnp.float32), precision=lax.Precision.HIGHEST)
        out_total = totals[1] + jnp.dot(heads_part.astype(jnp.float32).T, output_part.astype(jnp.float32), precision=lax.Precision.HIGHEST)
        return ((query_total, out_total), None)
    start_totals = (jnp.zeros((D, QW), jnp.float32), jnp.zeros((QW, D), jnp.float32))
    totals, unused = lax.scan(accumulate, start_totals, (inputs_blocks, query_blocks, heads_blocks, output_blocks))
    token_scale = TOKENS ** (-0.5)
    query_grad = totals[0] * token_scale
    out_grad = totals[1] * token_scale
    query_results = update_matrix(query_grad, query_basis, query_mean, query_square, query_weight)
    out_results = update_matrix(out_grad, out_basis, out_mean, out_square, out_weight)
    return (query_results[0], query_results[1], query_results[2], query_results[3], query_results[4], out_results[0], out_results[1], out_results[2], out_results[3], out_results[4])
```

```python
import functools

import jax
import jax.numpy as jnp
from jax import lax
from jax.experimental import pallas as pl
from jax.experimental.pallas import tpu as pltpu
from jax.sharding import PartitionSpec as P


VMEM = pl.BlockSpec(memory_space=pltpu.VMEM)
SMEM = pl.BlockSpec(memory_space=pltpu.SMEM)


class Grid:
    def __init__(self, mesh):
        devices = list(mesh.devices.reshape(-1))
        self.X = len({d.coords[0] for d in devices})
        self.Z = mesh.shape["fs"] // self.X
        self.Y = len({d.coords[1] for d in devices})
        self.C = mesh.shape["tp"] // self.Y

    def send(self, value, axis, shift):
        name = "fs" if axis in "zx" else "tp"
        inner = {"z": self.X, "x": 1, "y": self.C, "c": 1}[axis]
        size = {"z": self.Z, "x": self.X, "y": self.Y, "c": self.C}[axis]
        total = {"fs": self.Z * self.X, "tp": self.Y * self.C}[name]
        pairs = []
        for a in range(total):
            k = a // inner % size
            pairs.append((a, a + ((k + shift) % size - k) * inner))
        return lax.ppermute(value, name, pairs)


def gather_fs(g, own):
    column = jnp.stack([own] + [g.send(own, "z", dz) for dz in range(1, g.Z)])
    return [column] + [g.send(column, "x", dx) for dx in range(1, g.X)]


def project_kernel(g, at, left_in, right_in, *refs):
    n = g.X * g.C
    pieces, (basis, away, home, left, product) = refs[:n], refs[n:]
    z, x, y, c = at[0], at[1], at[2], at[3]
    half = pieces[0].shape[1]
    for dc in range(g.C):
        for dx in range(g.X):
            piece = pieces[dc * g.X + dx]
            for dz in range(g.Z):
                fs = lax.rem(z - dz + g.Z, g.Z) * g.X + lax.rem(x - dx + g.X, g.X)
                row = (fs * g.C + lax.rem(c - dc + g.C, g.C)) * half
                basis[pl.ds(pl.multiple_of(row, half), half), :] = piece[dz]
    tokens = left_in.shape[0]
    step = min(256, tokens)

    @pl.loop(0, tokens // step)
    def _(i):
        rows = pl.ds(pl.multiple_of(i * step, step), step)
        left[rows, :] = jnp.dot(
            left_in[rows, :], basis[...], preferred_element_type=jnp.float32
        ).astype(jnp.bfloat16)

    cols = home.shape[-1]
    rank_rows = home.shape[-2]
    for dc in range(g.C):
        for dy in range(g.Y):
            tp = lax.rem(y + dy, g.Y) * g.C + lax.rem(c + dc, g.C)
            columns = pl.ds(pl.multiple_of(tp * cols, cols), cols)
            product[...] = lax.dot_general(
                left[...],
                right_in[:, columns],
                (((0,), (0,)), ((), ())),
                preferred_element_type=jnp.float32,
            )
            for dx in range(g.X):
                for dz in range(g.Z):
                    fs = lax.rem(z + dz, g.Z) * g.X + lax.rem(x + dx, g.X)
                    block = product[pl.ds(pl.multiple_of(fs * rank_rows, rank_rows), rank_rows), :]
                    if dc:
                        away[dc - 1, dy, dx, dz] = block.astype(jnp.bfloat16)
                    else:
                        home[dy, dx, dz] = block


def project(g, at, left_in, right_in, pieces):
    rank = pieces[0].shape[-1]
    rows = left_in.shape[1]
    tokens = left_in.shape[0]
    cols = right_in.shape[1] // (g.Y * g.C)
    rank_rows = rank // (g.X * g.Z)
    blocks = (g.Y, g.X, g.Z, rank_rows, cols)
    return pl.pallas_call(
        functools.partial(project_kernel, g),
        out_shape=(
            jax.ShapeDtypeStruct((rows, rank), jnp.bfloat16),
            jax.ShapeDtypeStruct((g.C - 1, *blocks), jnp.bfloat16),
            jax.ShapeDtypeStruct(blocks, jnp.float32),
        ),
        in_specs=[SMEM] + [VMEM] * (2 + len(pieces)),
        out_specs=(VMEM, VMEM, VMEM),
        scratch_shapes=[
            pltpu.VMEM((tokens, rank), jnp.bfloat16),
            pltpu.VMEM((rank, cols), jnp.float32),
        ],
        cost_estimate=pl.CostEstimate(
            flops=2 * tokens * rank * (rows + right_in.shape[1]),
            bytes_accessed=2 * tokens * (rows + right_in.shape[1]),
            transcendentals=0,
        ),
    )(at, left_in, right_in, *pieces)


def reduce_rest(g, away, home):
    total = home
    for dc in range(1, g.C):
        total = total + g.send(away[dc - 1], "c", dc).astype(jnp.float32)
    for axis, size in (("y", g.Y), ("x", g.X), ("z", g.Z)):
        parts = [
            g.send(total[d].astype(jnp.bfloat16), axis, d) for d in range(1, size)
        ]
        total = total[0]
        for part in parts:
            total = total + part.astype(jnp.float32)
    return total


def moments(reduced, mean, square):
    mean_new = 0.8 * mean + 0.2 * reduced
    square_new = 0.9 * square + 0.1 * reduced * reduced
    direction = mean_new / (jnp.sqrt(square_new) + 1e-08)
    return (mean_new, square_new, direction)


def update_kernel(g, at, basis, weight, *refs):
    n = g.X
    directions, weights = refs[:n], refs[n : 2 * n]
    step_out, weight_out, copy_out, direction, full = refs[2 * n :]
    z, x = at[0], at[1]
    rank_rows = directions[0].shape[1]
    rows = weight.shape[0]
    cols = weight.shape[1]
    own = z * g.X + x
    for dx in range(g.X):
        for dz in range(g.Z):
            fs = lax.rem(z - dz + g.Z, g.Z) * g.X + lax.rem(x - dx + g.X, g.X)
            direction[pl.ds(pl.multiple_of(fs * rank_rows, rank_rows), rank_rows), :] = directions[dx][dz]

    def block(k, total):
        at_rows = pl.ds(pl.multiple_of(k * rows, rows), rows)
        value = jnp.dot(basis[at_rows, :], direction[...], preferred_element_type=jnp.float32)
        full[at_rows, :] = value
        return total + jnp.sum(value * value, axis=0, keepdims=True)

    squares = lax.fori_loop(0, g.X * g.Z, block, jnp.zeros((1, cols), jnp.float32))
    scale = lax.rsqrt(squares / (rows * g.X * g.Z) + 0.05)
    step = full[pl.ds(pl.multiple_of(own * rows, rows), rows), :] * scale
    step_out[...] = step
    new = weight[...] - 0.01 * step
    weight_out[...] = new
    for dx in range(g.X):
        for dz in range(g.Z):
            fs = lax.rem(z - dz + g.Z, g.Z) * g.X + lax.rem(x - dx + g.X, g.X)
            at_rows = pl.ds(pl.multiple_of(fs * rows, rows), rows)
            if dx == dz == 0:
                copy_out[at_rows, :] = new.astype(jnp.bfloat16)
            else:
                copy_out[at_rows, :] = (
                    weights[dx][dz].astype(jnp.float32) - 0.01 * (full[at_rows, :] * scale)
                ).astype(jnp.bfloat16)


def update(g, at, basis, weight, directions, weights):
    rank = basis.shape[1]
    rows, cols = weight.shape
    whole = basis.shape[0]
    return pl.pallas_call(
        functools.partial(update_kernel, g),
        out_shape=(
            jax.ShapeDtypeStruct((rows, cols), jnp.float32),
            jax.ShapeDtypeStruct((rows, cols), jnp.float32),
            jax.ShapeDtypeStruct((whole, cols), jnp.bfloat16),
        ),
        in_specs=[SMEM] + [VMEM] * (2 + len(directions) + len(weights)),
        out_specs=(VMEM, VMEM, VMEM),
        scratch_shapes=[
            pltpu.VMEM((rank, cols), jnp.bfloat16),
            pltpu.VMEM((whole, cols), jnp.float32),
        ],
        cost_estimate=pl.CostEstimate(
            flops=2 * whole * rank * cols, bytes_accessed=2 * whole * rank, transcendentals=0
        ),
    )(at, basis, weight, *directions, *weights)


def gather_basis(g, c, block):
    half = block.shape[0] // g.C
    own = lax.dynamic_slice_in_dim(block, c * half, half, axis=0)
    mine = gather_fs(g, own)
    both = jnp.stack(mine)
    pieces = list(mine)
    for dc in range(1, g.C):
        other = g.send(both, "c", dc)
        pieces += [other[dx] for dx in range(g.X)]
    return pieces


def shards(
    g,
    normed_inputs,
    query_cotangent,
    head_outputs,
    output_cotangent,
    query_weight,
    out_weight,
    query_basis,
    out_basis,
    query_mean,
    query_square,
    out_mean,
    out_square,
):
    tokens = normed_inputs.shape[0] * g.X * g.Z * g.Y * g.C
    token_scale = tokens ** (-0.5)
    fs, tp = lax.axis_index("fs"), lax.axis_index("tp")
    c = tp % g.C
    at = jnp.stack([fs // g.X, fs % g.X, tp // g.C, c]).astype(jnp.int32)
    out_pieces = gather_basis(g, c, out_basis)
    query_pieces = gather_basis(g, c, query_basis)
    out_low, query_low, unused = lax.optimization_barrier(
        (out_weight.astype(jnp.bfloat16), query_weight.astype(jnp.bfloat16), query_pieces[0])
    )
    out_weights = gather_fs(g, out_low)
    query_weights = gather_fs(g, query_low)

    out_all, out_away, out_home = project(g, at, head_outputs, output_cotangent, out_pieces)
    query_all, query_away, query_home = project(g, at, normed_inputs, query_cotangent, query_pieces)
    out_reduced = reduce_rest(g, out_away, out_home) * token_scale
    query_reduced = reduce_rest(g, query_away, query_home) * token_scale
    out_mean_new, out_square_new, out_direction = moments(out_reduced, out_mean, out_square)
    query_mean_new, query_square_new, query_direction = moments(
        query_reduced, query_mean, query_square
    )
    out_directions = gather_fs(g, out_direction.astype(jnp.bfloat16))
    query_directions = gather_fs(g, query_direction.astype(jnp.bfloat16))
    out_step, out_weight_new, out_copy = update(
        g, at, out_all, out_weight, out_directions, out_weights
    )
    query_step, query_weight_new, query_copy = update(
        g, at, query_all, query_weight, query_directions, query_weights
    )
    return (
        query_mean_new,
        query_square_new,
        query_step,
        query_weight_new,
        query_copy,
        out_mean_new,
        out_square_new,
        out_step,
        out_weight_new,
        out_copy,
    )


def solution(mesh):
    tokens, block, rows = P(("fs", "tp"), None), P("fs", "tp"), P("fs", None)
    columns = P(None, "tp")
    in_specs = (tokens,) * 4 + (block,) * 2 + (rows,) * 2 + (block,) * 4
    out_specs = (block, block, block, block, columns) * 2
    return jax.shard_map(
        functools.partial(shards, Grid(mesh)),
        mesh=mesh,
        in_specs=in_specs,
        out_specs=out_specs,
        check_vma=False,
    )
```
